32 devices in a mesh: grp: 2 (over y), fs: 4 (over z), tp: 4 (over x, core).
Axes of the slice: x: 2, y: 2, z: 4, core: 2. Of those that a mesh axis runs over, the one named last changes fastest.
Arguments:
- tokens: bfloat16 [4096, 2048], P(('grp', 'fs')), parts along dimension 0, may hold values from -6 to 6
- pre_gain: float32 [2048], replicated, may hold values from 0.1 to 1.9
- gate_weight: float32 [2048, 5632], P('fs', 'tp'), may hold values from -0.125 to 0.125
- gate_scale: float32 [5632], P('tp'), may hold values from 0.5 to 2
- up_weight: float32 [2048, 5632], P('fs', 'tp'), may hold values from -0.125 to 0.125
- up_scale: float32 [5632], P('tp'), may hold values from 0.5 to 2
- down_weight: float32 [5632, 2048], P('tp', 'fs'), may hold values from -0.078125 to 0.078125
- down_scale: float32 [2048], replicated, may hold values from 0.3 to 3
- post_gain: float32 [2048], replicated, may hold values from 0.1 to 1.9
Outputs:
- mixed: bfloat16 [4096, 2048], P(('grp', 'fs')), parts along dimension 0
The draws below stay inside these ranges and needn't reach their ends.
There are 2 independent parts, one for each index of `grp`. The reference program is written for one: setup_inputs(seed, part) draws one part's arguments, and reference() takes and returns one part's arrays. A program takes and returns all parts, laid end to end along the dimension named above; an argument that names none is the same for every part. Nothing has to cross between parts.
All inputs are finite; a program needn't handle non-finite values.
Results may differ from the reference program's by a relative error of at most 0.018.
Values may be sent and summed in bfloat16 or wider, within the bound.
A program may use at most 64 MiB of HBM per device.

```python
import math
import jax
import jax.numpy as jnp
from jax import lax

D = 2048
FF = 5632
TOKENS = 2048
N_TP = 4


def shard_levels(stream_key, dims, pieces, least, high):
    def one(dim, shards_of):
        draws = jax.random.uniform(jax.random.fold_in(jax.random.fold_in(stream_key, 6), dim), (shards_of,), jnp.float32, least / len(pieces), high / len(pieces))
        return jnp.repeat(jnp.exp(draws), dims[dim] // shards_of).reshape((-1,) + (1,) * (len(dims) - dim - 1))

    level = one(*pieces[0])
    for cut in pieces[1:]:
        level = level * one(*cut)
    return level


def bell_draw(key, shape, scale, reach, shards=(), held_as=jnp.bfloat16):
    factor_of = shard_levels(key, shape, shards, -0.22, 0.18) if shards else 1.0
    array = jax.random.normal(key, shape, jnp.float32) * scale * factor_of
    return jnp.minimum(jnp.maximum(array, -reach), reach).astype(held_as)


def setup_inputs(seed: int = 0, part: int = 0) -> dict:
    splits = jax.random.split(jax.random.key(seed), 10)
    part_keys = jax.random.split(jax.random.fold_in(splits[9], part), 10)
    return {
        "tokens": bell_draw(part_keys[0], (TOKENS, D), 1.0, 6.0, ((0, 4),)),
        "pre_gain": jnp.clip(1.0 + 0.18 * jax.random.normal(splits[1], (D,), jnp.float32), 0.1, 1.9),
        "gate_weight": bell_draw(splits[2], (D, FF), D ** -0.5, 0.125, ((0, 4), (1, 4)), jnp.float32),
        "gate_scale": jnp.clip(jnp.exp(math.log(2.0) - 1.3862944 * jax.random.uniform(splits[3], (FF,), jnp.float32) ** shard_levels(splits[3], (FF,), ((0, 4),), -0.2, 0.2)), 0.5, 2.0),
        "up_weight": bell_draw(splits[4], (D, FF), D ** -0.5, 0.125, ((0, 4), (1, 4)), jnp.float32),
        "up_scale": jnp.clip(jnp.exp(math.log(2.0) - 1.3862944 * jax.random.uniform(splits[5], (FF,), jnp.float32) ** shard_levels(splits[5], (FF,), ((0, 4),), -0.2, 0.2)), 0.5, 2.0),
        "down_weight": bell_draw(splits[6], (FF, D), FF ** -0.5, 0.078125, ((0, 4), (1, 4)), jnp.float32),
        "down_scale": jnp.clip(jnp.exp(jax.random.uniform(splits[7], (D,), jnp.float32, math.log(0.3), math.log(3.0))), 0.3, 3.0),
        "post_gain": jnp.clip(1.0 + 0.18 * jax.random.normal(splits[8], (D,), jnp.float32), 0.1, 1.9),
    }


EPS = 1e-06

def reference(tokens, pre_gain, gate_weight, gate_scale, up_weight, up_scale, down_weight, down_scale, post_gain):
    rows = tokens.astype(jnp.float32)
    normed = (rows * lax.rsqrt(lax.optimization_barrier(jnp.mean(rows * rows, axis=-1, keepdims=True)) + EPS) * pre_gain).astype(jnp.bfloat16)
    gate_low = gate_weight.astype(jnp.bfloat16)
    up_low = up_weight.astype(jnp.bfloat16)
    down_low = down_weight.astype(jnp.bfloat16)
    gate = jnp.dot(normed, gate_low, preferred_element_type=jnp.float32) * gate_scale
    up = jnp.dot(normed, up_low, preferred_element_type=jnp.float32) * up_scale
    hidden = (jax.nn.silu(gate) * up).astype(jnp.bfloat16)
    width = FF // N_TP
    hidden_blocks = jnp.transpose(hidden.reshape(hidden.shape[0], N_TP, width), (1, 0, 2))
    down_blocks = down_low.reshape(N_TP, width, down_low.shape[1])

    def accumulate(total, pair):
        part = jnp.dot(pair[0], pair[1], preferred_element_type=jnp.float32).astype(jnp.bfloat16)
        return (total + part.astype(jnp.float32), None)
    start = jnp.zeros((hidden.shape[0], down_low.shape[1]), jnp.float32)
    summed, unused = lax.scan(accumulate, start, (hidden_blocks, down_blocks))
    branch = summed * down_scale
    scaled = branch * lax.rsqrt(lax.optimization_barrier(jnp.mean(branch * branch, axis=-1, keepdims=True)) + EPS) * post_gain
    return scaled.astype(jnp.bfloat16)
```

```python
import jax
import jax.numpy as jnp
from jax import lax
from jax.sharding import PartitionSpec as P

EPS = 1e-06


def finish(summed, down_scale, post_gain):
    branch = summed * down_scale
    return (
        branch * lax.rsqrt(jnp.mean(branch * branch, axis=-1, keepdims=True) + EPS) * post_gain
    ).astype(jnp.bfloat16)


def gather_shards(block):
    groups, shards = lax.axis_size("grp"), lax.axis_size("fs")
    rows, columns = block.shape
    pieces = block.reshape(groups, rows // groups, columns)
    mine = lax.dynamic_index_in_dim(pieces, lax.axis_index("grp"), 0, keepdims=False)
    whole = lax.all_gather(mine, ("fs", "grp"), axis=0, tiled=True)
    return whole.reshape(shards, rows, columns)


def gather_shared(block):
    whole = gather_shards(block)
    return whole.reshape(-1, block.shape[1])


def body(
    tokens,
    pre_gain,
    gate_weight,
    gate_scale,
    up_weight,
    up_scale,
    down_weight,
    down_scale,
    post_gain,
):
    rows = tokens.astype(jnp.float32)
    normed = (
        rows * lax.rsqrt(jnp.mean(rows * rows, axis=-1, keepdims=True) + EPS) * pre_gain
    ).astype(jnp.bfloat16)
    gate_low = gate_weight.astype(jnp.bfloat16)
    up_low = up_weight.astype(jnp.bfloat16)
    down_low = down_weight.astype(jnp.bfloat16)
    gate_full, up_full = gather_shared(gate_low), gather_shared(up_low)
    gate = jnp.dot(normed, gate_full, preferred_element_type=jnp.float32) * gate_scale
    up = jnp.dot(normed, up_full, preferred_element_type=jnp.float32) * up_scale
    hidden = (jax.nn.silu(gate) * up).astype(jnp.bfloat16)
    shards = gather_shards(down_low)
    partial_value = jnp.concatenate(
        [jnp.dot(hidden, shards[k], preferred_element_type=jnp.float32) for k in range(shards.shape[0])], axis=1
    )
    summed = lax.psum(partial_value.astype(jnp.bfloat16), "tp").astype(jnp.float32)
    return finish(summed, down_scale, post_gain)


def solution(mesh):
    in_specs = (
        P(("grp", "fs"), None),
        P(),
        P("fs", "tp"),
        P("tp"),
        P("fs", "tp"),
        P("tp"),
        P("tp", "fs"),
        P(),
        P(),
    )
    out_specs = P(("grp", "fs"), None)
    return jax.shard_map(body, mesh=mesh, in_specs=in_specs, out_specs=out_specs, check_vma=False)
```

```python
import functools

import jax
import jax.numpy as jnp
from jax import lax
from jax.experimental import pallas as pl
from jax.experimental.pallas import tpu as pltpu
from jax.sharding import PartitionSpec as P

EPS = 1e-06
LANES = 128
ORDER = (0, 1, 3, 2)


def up_to(value, step):
    return -(-value // step) * step


def fused(
    sizes, pieces_ref, token_ref, scale_ref, gain_ref, out_ref,
    held, toks, acc, hid, part, red,
    own_sem, got, sent_z, sent_x, sent_y, sent_s,
    tok_own, tok_got, tok_sent, red_got, red_sent, out_got, out_sent,
):
    unit, block, half, width = sizes
    n_y, n_z, n_t = held.shape[:3]
    y, z, t = lax.axis_index("grp"), lax.axis_index("fs"), lax.axis_index("tp")
    x, c = t // 2, t % 2
    t_x, t_s, t_d = (1 - x) * 2 + c, x * 2 + 1 - c, (1 - x) * 2 + 1 - c
    y_o = 1 - y
    xn, yn, sn = {"tp": t_x}, {"grp": y_o}, {"tp": t_s}

    barrier = pltpu.get_barrier_semaphore()
    peers = [{"fs": (z + d) % n_z} for d in range(1, n_z)] + [xn, yn, sn]
    for peer in peers:
        pl.semaphore_signal(barrier, inc=1, device_id=peer, device_id_type=pl.DeviceIdType.MESH)
    pl.semaphore_wait(barrier, len(peers))

    pending = []

    def send(src, dst, s_sem, r_sem, to):
        copy = pltpu.make_async_remote_copy(
            src_ref=src, dst_ref=dst, send_sem=s_sem, recv_sem=r_sem,
            device_id=to, device_id_type=pl.DeviceIdType.MESH,
        )
        copy.start()
        return copy

    def pass_on(slot, sems, to):
        pending.append(send(held.at[slot], held.at[slot], sems.at[slot], got.at[slot], to))

    def arrived(slot):
        pltpu.make_async_remote_copy(
            src_ref=held.at[slot], dst_ref=held.at[slot], send_sem=sent_s.at[slot], recv_sem=got.at[slot],
            device_id=sn, device_id_type=pl.DeviceIdType.MESH,
        ).wait_recv()

    own = pltpu.make_async_copy(pieces_ref.at[z], held.at[y, z, t], own_sem)
    own.start()
    own_tok = pltpu.make_async_copy(token_ref, toks.at[z], tok_own)
    own_tok.start()

    def send_piece(d):
        to = (z + d) % n_z
        pending.append(send(pieces_ref.at[to], held.at[y, z, t], sent_z.at[d], got.at[y, z, t], {"fs": to}))

    def token_copy(src, slot, side):
        return pltpu.make_async_remote_copy(
            src_ref=src, dst_ref=toks.at[slot], send_sem=tok_sent.at[slot, side], recv_sem=tok_got.at[slot],
            device_id={"fs": (z + 1 if side else z - 1 + n_z) % n_z}, device_id_type=pl.DeviceIdType.MESH,
        )

    send_piece(ORDER[1])
    for side in (0, 1):
        @pl.when((z < n_z - 1) if side else (z > 0))
        def _():
            token_copy(token_ref, z, side).start()
    for d in ORDER[2:]:
        send_piece(d)

    def zs_of(i):
        return (z - ORDER[i] + n_z) % n_z

    def first(i):
        slot = (y, zs_of(i), t)
        if i == 0:
            own.wait()
        else:
            arrived(slot)
        pass_on(slot, sent_x, xn)
        pass_on(slot, sent_y, yn)
        pass_on(slot, sent_s, sn)

    def second(i):
        zs = zs_of(i)
        slot = (y, zs, t_x)
        arrived(slot)
        if i % 2 == 0:
            pass_on(slot, sent_y, yn)
        pass_on(slot, sent_s, sn)
        slot = (y_o, zs, t)
        arrived(slot)
        if i % 2 == 1:
            pass_on(slot, sent_x, xn)
        pass_on(slot, sent_s, sn)

    def third(i):
        slot = (y_o, zs_of(i), t_x)
        arrived(slot)
        pass_on(slot, sent_s, sn)

    def siblings(i):
        zs = zs_of(i)
        for q, tt in ((y, t_s), (y, t_d), (y_o, t_s), (y_o, t_d)):
            arrived((q, zs, tt))

    def multiply(i):
        zs = zs_of(i)

        @pl.loop(0, n_t)
        def _(tt):
            for q in range(n_y):
                columns = pl.ds(pl.multiple_of((zs * n_y + q) * half, half), half)
                rows = toks[:, :, columns].reshape(-1, half)
                weight = jnp.concatenate(
                    [held[q, zs, tt, pl.ds(k * half, half), :] for k in range(2 * block // LANES)], axis=1
                )
                value = jnp.dot(rows, weight, preferred_element_type=jnp.float32)
                if i == 0 and q == 0:
                    acc[tt] = value
                else:
                    acc[tt] += value

    def tokens_on():
        for k in range(1, n_z):
            for side in (0, 1):
                here = (z - k >= 0) if side else (z + k < n_z)

                @pl.when(here)
                def _():
                    slot = (z - k if side else z + k) % n_z
                    token_copy(toks.at[slot], slot, side).wait_recv()

                    @pl.when((z + 1 < n_z) if side else (z > 0))
                    def _():
                        token_copy(toks.at[slot], slot, side).start()

    first(0)
    own_tok.wait()
    first(1)
    second(0)
    tokens_on()
    first(2)
    third(0)
    second(1)
    siblings(0)
    multiply(0)
    first(3)
    third(1)
    second(2)
    siblings(1)
    multiply(1)
    second(3)
    third(2)
    siblings(2)
    multiply(2)
    third(3)
    siblings(3)
    multiply(3)

    @pl.loop(0, n_t)
    def _(tt):
        gate, up = acc[tt, :, :block], acc[tt, :, block:]
        hid[tt] = (gate / (1.0 + jnp.exp(-gate)) * up).astype(jnp.bfloat16)[:, :unit]

    base = 2 * block // LANES * half
    fan = half // LANES
    red_sends = []
    for zs in range(n_z):
        for q in range(n_y):
            total = None
            for tt in range(n_t):
                weight = jnp.concatenate(
                    [held[q, zs, tt, pl.ds(base + k * unit, unit), :] for k in range(fan)], axis=1
                )
                value = jnp.dot(hid[tt], weight, preferred_element_type=jnp.float32)
                total = value if total is None else total + value
            part[:, :, pl.ds((zs * n_y + q) * half, half)] = total.astype(jnp.bfloat16).reshape(n_z, -1, half)
        columns = pl.ds(zs * n_y * half, n_y * half)
        for d in ORDER[1:]:
            to = (z + d) % n_z
            red_sends.append(send(
                part.at[to, :, columns], red.at[d, :, columns],
                red_sent.at[d, zs], red_got.at[d, zs], {"fs": to},
            ))
    for copy in red_sends:
        copy.wait_recv()
    summed = part[z].astype(jnp.float32)
    for d in range(1, n_z):
        summed += red[d].astype(jnp.float32)
    branch = summed * scale_ref[...]
    mean = jnp.mean(branch * branch, axis=-1, keepdims=True)
    out_ref[t] = (branch * lax.rsqrt(mean + EPS) * gain_ref[...]).astype(jnp.bfloat16)

    def give(slot, k, to):
        pending.append(send(out_ref.at[slot], out_ref.at[slot], out_sent.at[k], out_got.at[slot], to))

    def taken(slot):
        pltpu.make_async_remote_copy(
            src_ref=out_ref.at[slot], dst_ref=out_ref.at[slot], send_sem=out_sent.at[0], recv_sem=out_got.at[slot],
            device_id=sn, device_id_type=pl.DeviceIdType.MESH,
        ).wait_recv()

    give(t, 0, xn)
    give(t, 1, sn)
    taken(t_x)
    give(t_x, 2, sn)
    taken(t_s)
    taken(t_d)
    for copy in pending + red_sends:
        copy.wait_send()
    for side in (0, 1):
        for k in range(0, n_z):
            origin = (z - k >= 0) if side else (z + k < n_z)

            @pl.when(origin & ((z + 1 < n_z) if side else (z > 0)))
            def _():
                slot = (z - k if side else z + k) % n_z
                token_copy(toks.at[slot], slot, side).wait_send()


def quad_body(
    tokens, pre_gain, gate_weight, gate_scale, up_weight, up_scale, down_weight, down_scale, post_gain,
):
    n_y, n_z, n_t = (lax.axis_size(a) for a in ("grp", "fs", "tp"))
    y, t = lax.axis_index("grp"), lax.axis_index("tp")
    shard, hidden = gate_weight.shape
    unit, half = hidden // n_z, shard // n_y
    block = up_to(unit, LANES)
    share, width = tokens.shape[0] // n_t, tokens.shape[1]

    rows = lax.dynamic_slice_in_dim(tokens, t * share, share, 0).astype(jnp.float32)
    normed = (
        rows * lax.rsqrt(jnp.mean(rows * rows, axis=-1, keepdims=True) + EPS) * pre_gain
    ).astype(jnp.bfloat16)

    def pieces_of(weight, scale):
        mine = lax.dynamic_slice_in_dim(weight, y * half, half, 0)
        low = (mine * scale).astype(jnp.bfloat16).reshape(half, n_z, unit)
        low = jnp.pad(low, ((0, 0), (0, 0), (0, block - unit)))
        return low.reshape(half, n_z, block // LANES, LANES).transpose(1, 2, 0, 3).reshape(n_z, -1, LANES)

    mine = lax.dynamic_slice_in_dim(down_weight, y * half, half, 1).astype(jnp.bfloat16)
    low = mine.reshape(n_z, unit, half // LANES, LANES).transpose(0, 2, 1, 3).reshape(n_z, -1, LANES)
    pieces = jnp.concatenate(
        [pieces_of(gate_weight, gate_scale), pieces_of(up_weight, up_scale), low], axis=1
    )
    depth = pieces.shape[1]
    bf16, f32, dma = jnp.bfloat16, jnp.float32, pltpu.SemaphoreType.DMA
    slots = (n_y, n_z, n_t)
    vmem = pl.BlockSpec(memory_space=pltpu.VMEM)
    out = pl.pallas_call(
        functools.partial(fused, (unit, block, half, width)),
        out_shape=jax.ShapeDtypeStruct((n_t, share, width), bf16),
        in_specs=[vmem] * 4,
        out_specs=vmem,
        scratch_shapes=[
            pltpu.VMEM(slots + (depth, LANES), bf16),
            pltpu.VMEM((n_z, share, width), bf16),
            pltpu.VMEM((n_t, n_z * share, 2 * block), f32),
            pltpu.VMEM((n_t, n_z * share, unit), bf16),
            pltpu.VMEM((n_z, share, width), bf16),
            pltpu.VMEM((n_z, share, width), bf16),
            dma, dma(slots), dma((n_z,)), dma(slots), dma(slots), dma(slots),
            dma, dma((n_z,)), dma((n_z, 2)), dma((n_z, n_z)), dma((n_z, n_z)), dma((n_t,)), dma((3,)),
        ],
        compiler_params=pltpu.CompilerParams(
            collective_id=0, has_side_effects=True, vmem_limit_bytes=60 * 2**20
        ),
    )(pieces, normed, down_scale[None], post_gain[None])
    return out.reshape(n_t * share, width)


def finish(summed, down_scale, post_gain):
    branch = summed * down_scale
    return (
        branch * lax.rsqrt(jnp.mean(branch * branch, axis=-1, keepdims=True) + EPS) * post_gain
    ).astype(jnp.bfloat16)


def gather_shards(block):
    groups, shards = lax.axis_size("grp"), lax.axis_size("fs")
    rows, columns = block.shape
    pieces = block.reshape(groups, rows // groups, columns)
    mine = lax.dynamic_index_in_dim(pieces, lax.axis_index("grp"), 0, keepdims=False)
    whole = lax.all_gather(mine, ("fs", "grp"), axis=0, tiled=True)
    return whole.reshape(shards, rows, columns)


def gather_shared(block):
    whole = gather_shards(block)
    return whole.reshape(-1, block.shape[1])


def body(
    tokens,
    pre_gain,
    gate_weight,
    gate_scale,
    up_weight,
    up_scale,
    down_weight,
    down_scale,
    post_gain,
):
    rows = tokens.astype(jnp.float32)
    normed = (
        rows * lax.rsqrt(jnp.mean(rows * rows, axis=-1, keepdims=True) + EPS) * pre_gain
    ).astype(jnp.bfloat16)
    gate_low = gate_weight.astype(jnp.bfloat16)
    up_low = up_weight.astype(jnp.bfloat16)
    down_low = down_weight.astype(jnp.bfloat16)
    gate_full, up_full = gather_shared(gate_low), gather_shared(up_low)
    gate = jnp.dot(normed, gate_full, preferred_element_type=jnp.float32) * gate_scale
    up = jnp.dot(normed, up_full, preferred_element_type=jnp.float32) * up_scale
    hidden = (jax.nn.silu(gate) * up).astype(jnp.bfloat16)
    shards = gather_shards(down_low)
    partial_value = jnp.concatenate(
        [jnp.dot(hidden, shards[k], preferred_element_type=jnp.float32) for k in range(shards.shape[0])], axis=1
    )
    summed = lax.psum(partial_value.astype(jnp.bfloat16), "tp").astype(jnp.float32)
    return finish(summed, down_scale, post_gain)


def solution(mesh):
    in_specs = (
        P(("grp", "fs"), None),
        P(),
        P("fs", "tp"),
        P("tp"),
        P("fs", "tp"),
        P("tp"),
        P("tp", "fs"),
        P(),
        P(),
    )
    out_specs = P(("grp", "fs"), None)
    sizes = tuple(mesh.shape[a] for a in ("grp", "fs", "tp"))
    chosen = quad_body if sizes == (2, 4, 4) else body
    return jax.shard_map(chosen, mesh=mesh, in_specs=in_specs, out_specs=out_specs, check_vma=False)
```

```python
import functools

import jax
import jax.numpy as jnp
from jax import lax
from jax.experimental import pallas as pl
from jax.experimental.pallas import tpu as pltpu
from jax.sharding import PartitionSpec as P

EPS = 1e-06
LANES = 128
ORDER = (0, 1, 3, 2)


def up_to(value, step):
    return -(-value // step) * step


def fused(
    sizes, gate_ref, up_ref, down_ref, token_ref, scale_ref, gain_ref, out_ref,
    pieces_ref, held, toks, acc, hid, part, red,
    own_sem, got, sent_z, sent_x, sent_y, sent_s,
    tok_own, tok_got, tok_sent, red_got, red_sent, out_got, out_sent,
):
    unit, block, half, width = sizes
    n_y, n_z, n_t = held.shape[:3]
    y, z, t = lax.axis_index("grp"), lax.axis_index("fs"), lax.axis_index("tp")
    x, c = t // 2, t % 2
    t_x, t_s, t_d = (1 - x) * 2 + c, x * 2 + 1 - c, (1 - x) * 2 + 1 - c
    y_o = 1 - y
    xn, yn, sn = {"tp": t_x}, {"grp": y_o}, {"tp": t_s}

    barrier = pltpu.get_barrier_semaphore()
    peers = [{"fs": (z + d) % n_z} for d in range(1, n_z)] + [xn, yn, sn]
    for peer in peers:
        pl.semaphore_signal(barrier, inc=1, device_id=peer, device_id_type=pl.DeviceIdType.MESH)
    for k in range(n_z):
        for j, ref in enumerate((gate_ref, up_ref)):
            for b in range(block // LANES):
                lanes = min(LANES, unit - b * LANES)
                rows = pl.ds((j * (block // LANES) + b) * half, half)
                pieces_ref[k, rows, :lanes] = ref[:, k * unit + b * LANES:k * unit + b * LANES + lanes]
                if lanes < LANES:
                    pieces_ref[k, rows, lanes:] = jnp.zeros((half, LANES - lanes), jnp.bfloat16)
        for b in range(half // LANES):
            pieces_ref[k, pl.ds(2 * block // LANES * half + b * unit, unit), :] = down_ref[
                k * unit:(k + 1) * unit, b * LANES:(b + 1) * LANES
            ]
    pl.semaphore_wait(barrier, len(peers))

    pending = []

    def send(src, dst, s_sem, r_sem, to):
        copy = pltpu.make_async_remote_copy(
            src_ref=src, dst_ref=dst, send_sem=s_sem, recv_sem=r_sem,
            device_id=to, device_id_type=pl.DeviceIdType.MESH,
        )
        copy.start()
        return copy

    def pass_on(slot, sems, to):
        pending.append(send(held.at[slot], held.at[slot], sems.at[slot], got.at[slot], to))

    def arrived(slot):
        pltpu.make_async_remote_copy(
            src_ref=held.at[slot], dst_ref=held.at[slot], send_sem=sent_s.at[slot], recv_sem=got.at[slot],
            device_id=sn, device_id_type=pl.DeviceIdType.MESH,
        ).wait_recv()

    own = pltpu.make_async_copy(pieces_ref.at[z], held.at[y, z, t], own_sem)
    own.start()
    own_tok = pltpu.make_async_copy(token_ref, toks.at[z], tok_own)
    own_tok.start()

    def send_piece(d):
        to = (z + d) % n_z
        pending.append(send(pieces_ref.at[to], held.at[y, z, t], sent_z.at[d], got.at[y, z, t], {"fs": to}))

    def token_copy(src, slot, side):
        return pltpu.make_async_remote_copy(
            src_ref=src, dst_ref=toks.at[slot], send_sem=tok_sent.at[slot, side], recv_sem=tok_got.at[slot],
            device_id={"fs": (z + 1 if side else z - 1 + n_z) % n_z}, device_id_type=pl.DeviceIdType.MESH,
        )

    for side in (0, 1):
        @pl.when((z < n_z - 1) if side else (z > 0))
        def _():
            token_copy(token_ref, z, side).start()
    send_piece(ORDER[1])

    def zs_of(i):
        return (z - ORDER[i] + n_z) % n_z

    def first(i):
        slot = (y, zs_of(i), t)
        if i == 0:
            own.wait()
        else:
            arrived(slot)
        pass_on(slot, sent_x, xn)
        pass_on(slot, sent_y, yn)
        pass_on(slot, sent_s, sn)

    def second(i):
        zs = zs_of(i)
        slot = (y, zs, t_x)
        arrived(slot)
        if i % 2 == 0:
            pass_on(slot, sent_y, yn)
        pass_on(slot, sent_s, sn)
        slot = (y_o, zs, t)
        arrived(slot)
        if i % 2 == 1:
            pass_on(slot, sent_x, xn)
        pass_on(slot, sent_s, sn)

    def third(i):
        slot = (y_o, zs_of(i), t_x)
        arrived(slot)
        pass_on(slot, sent_s, sn)

    def siblings(i):
        zs = zs_of(i)
        for q, tt in ((y, t_s), (y, t_d), (y_o, t_s), (y_o, t_d)):
            arrived((q, zs, tt))

    def multiply(i):
        zs = zs_of(i)

        @pl.loop(0, n_t)
        def _(tt):
            for q in range(n_y):
                columns = pl.ds(pl.multiple_of((zs * n_y + q) * half, half), half)
                rows = toks[:, :, columns].reshape(-1, half)
                weight = jnp.concatenate(
                    [held[q, zs, tt, pl.ds(k * half, half), :] for k in range(2 * block // LANES)], axis=1
                )
                value = jnp.dot(rows, weight, preferred_element_type=jnp.float32)
                if i == 0 and q == 0:
                    acc[tt] = value
                else:
                    acc[tt] += value

    def tokens_on(k):
        for side in (0, 1):
            here = (z - k >= 0) if side else (z + k < n_z)

            @pl.when(here)
            def _():
                slot = (z - k if side else z + k) % n_z
                token_copy(toks.at[slot], slot, side).wait_recv()

                @pl.when((z + 1 < n_z) if side else (z > 0))
                def _():
                    token_copy(toks.at[slot], slot, side).start()

    first(0)
    own_tok.wait()
    tokens_on(1)
    send_piece(ORDER[2])
    second(0)
    first(1)
    tokens_on(2)
    send_piece(ORDER[3])
    third(0)
    second(1)
    first(2)
    third(1)
    tokens_on(3)
    siblings(0)
    multiply(0)
    second(2)
    first(3)
    siblings(1)
    multiply(1)
    third(2)
    second(3)
    siblings(2)
    multiply(2)
    third(3)
    siblings(3)
    multiply(3)

    @pl.loop(0, n_t)
    def _(tt):
        gate, up = acc[tt, :, :block], acc[tt, :, block:]
        hid[tt] = (gate / (1.0 + jnp.exp(-gate)) * up).astype(jnp.bfloat16)[:, :unit]

    base = 2 * block // LANES * half
    fan = half // LANES
    red_sends = []
    for zs in range(n_z):
        for q in range(n_y):
            total = None
            for tt in range(n_t):
                weight = jnp.concatenate(
                    [held[q, zs, tt, pl.ds(base + k * unit, unit), :] for k in range(fan)], axis=1
                )
                value = jnp.dot(hid[tt], weight, preferred_element_type=jnp.float32)
                total = value if total is None else total + value
            part[:, :, pl.ds((zs * n_y + q) * half, half)] = total.astype(jnp.bfloat16).reshape(n_z, -1, half)
        columns = pl.ds(zs * n_y * half, n_y * half)
        for d in ORDER[1:]:
            to = (z + d) % n_z
            red_sends.append(send(
                part.at[to, :, columns], red.at[d, :, columns],
                red_sent.at[d, zs], red_got.at[d, zs], {"fs": to},
            ))
    for copy in red_sends:
        copy.wait_recv()
    summed = part[z].astype(jnp.float32)
    for d in range(1, n_z):
        summed += red[d].astype(jnp.float32)
    branch = summed * scale_ref[...]
    mean = jnp.mean(branch * branch, axis=-1, keepdims=True)
    out_ref[t] = (branch * lax.rsqrt(mean + EPS) * gain_ref[...]).astype(jnp.bfloat16)

    def give(slot, k, to):
        pending.append(send(out_ref.at[slot], out_ref.at[slot], out_sent.at[k], out_got.at[slot], to))

    def taken(slot):
        pltpu.make_async_remote_copy(
            src_ref=out_ref.at[slot], dst_ref=out_ref.at[slot], send_sem=out_sent.at[0], recv_sem=out_got.at[slot],
            device_id=sn, device_id_type=pl.DeviceIdType.MESH,
        ).wait_recv()

    give(t, 0, xn)
    give(t, 1, sn)
    taken(t_x)
    give(t_x, 2, sn)
    taken(t_s)
    taken(t_d)
    for copy in pending + red_sends:
        copy.wait_send()
    for side in (0, 1):
        for k in range(0, n_z):
            origin = (z - k >= 0) if side else (z + k < n_z)

            @pl.when(origin & ((z + 1 < n_z) if side else (z > 0)))
            def _():
                slot = (z - k if side else z + k) % n_z
                token_copy(toks.at[slot], slot, side).wait_send()


def quad_body(
    tokens, pre_gain, gate_weight, gate_scale, up_weight, up_scale, down_weight, down_scale, post_gain,
):
    n_y, n_z, n_t = (lax.axis_size(a) for a in ("grp", "fs", "tp"))
    y, t = lax.axis_index("grp"), lax.axis_index("tp")
    shard, hidden = gate_weight.shape
    unit, half = hidden // n_z, shard // n_y
    block = up_to(unit, LANES)
    share, width = tokens.shape[0] // n_t, tokens.shape[1]

    rows = lax.dynamic_slice_in_dim(tokens, t * share, share, 0).astype(jnp.float32)
    normed = (
        rows * lax.rsqrt(jnp.mean(rows * rows, axis=-1, keepdims=True) + EPS) * pre_gain
    ).astype(jnp.bfloat16)

    def half_of(weight, axis):
        return lax.dynamic_slice_in_dim(weight, y * half, half, axis)

    gate_low = (half_of(gate_weight, 0) * gate_scale).astype(jnp.bfloat16)
    up_low = (half_of(up_weight, 0) * up_scale).astype(jnp.bfloat16)
    down_low = half_of(down_weight, 1).astype(jnp.bfloat16)
    depth = (2 * block * half + unit * half) // LANES
    bf16, f32, dma = jnp.bfloat16, jnp.float32, pltpu.SemaphoreType.DMA
    slots = (n_y, n_z, n_t)
    vmem = pl.BlockSpec(memory_space=pltpu.VMEM)
    out = pl.pallas_call(
        functools.partial(fused, (unit, block, half, width)),
        out_shape=jax.ShapeDtypeStruct((n_t, share, width), bf16),
        in_specs=[vmem] * 6,
        out_specs=vmem,
        scratch_shapes=[
            pltpu.VMEM((n_z, depth, LANES), bf16),
            pltpu.VMEM(slots + (depth, LANES), bf16),
            pltpu.VMEM((n_z, share, width), bf16),
            pltpu.VMEM((n_t, n_z * share, 2 * block), f32),
            pltpu.VMEM((n_t, n_z * share, unit), bf16),
            pltpu.VMEM((n_z, share, width), bf16),
            pltpu.VMEM((n_z, share, width), bf16),
            dma, dma(slots), dma((n_z,)), dma(slots), dma(slots), dma(slots),
            dma, dma((n_z,)), dma((n_z, 2)), dma((n_z, n_z)), dma((n_z, n_z)), dma((n_t,)), dma((3,)),
        ],
        compiler_params=pltpu.CompilerParams(
            collective_id=0, has_side_effects=True, vmem_limit_bytes=60 * 2**20
        ),
    )(gate_low, up_low, down_low, normed, down_scale[None], post_gain[None])
    return out.reshape(n_t * share, width)


def finish(summed, down_scale, post_gain):
    branch = summed * down_scale
    return (
        branch * lax.rsqrt(jnp.mean(branch * branch, axis=-1, keepdims=True) + EPS) * post_gain
    ).astype(jnp.bfloat16)


def gather_shards(block):
    groups, shards = lax.axis_size("grp"), lax.axis_size("fs")
    rows, columns = block.shape
    pieces = block.reshape(groups, rows // groups, columns)
    mine = lax.dynamic_index_in_dim(pieces, lax.axis_index("grp"), 0, keepdims=False)
    whole = lax.all_gather(mine, ("fs", "grp"), axis=0, tiled=True)
    return whole.reshape(shards, rows, columns)


def gather_shared(block):
    whole = gather_shards(block)
    return whole.reshape(-1, block.shape[1])


def body(
    tokens,
    pre_gain,
    gate_weight,
    gate_scale,
    up_weight,
    up_scale,
    down_weight,
    down_scale,
    post_gain,
):
    rows = tokens.astype(jnp.float32)
    normed = (
        rows * lax.rsqrt(jnp.mean(rows * rows, axis=-1, keepdims=True) + EPS) * pre_gain
    ).astype(jnp.bfloat16)
    gate_low = gate_weight.astype(jnp.bfloat16)
    up_low = up_weight.astype(jnp.bfloat16)
    down_low = down_weight.astype(jnp.bfloat16)
    gate_full, up_full = gather_shared(gate_low), gather_shared(up_low)
    gate = jnp.dot(normed, gate_full, preferred_element_type=jnp.float32) * gate_scale
    up = jnp.dot(normed, up_full, preferred_element_type=jnp.float32) * up_scale
    hidden = (jax.nn.silu(gate) * up).astype(jnp.bfloat16)
    shards = gather_shards(down_low)
    partial_value = jnp.concatenate(
        [jnp.dot(hidden, shards[k], preferred_element_type=jnp.float32) for k in range(shards.shape[0])], axis=1
    )
    summed = lax.psum(partial_value.astype(jnp.bfloat16), "tp").astype(jnp.float32)
    return finish(summed, down_scale, post_gain)


def solution(mesh):
    in_specs = (
        P(("grp", "fs"), None),
        P(),
        P("fs", "tp"),
        P("tp"),
        P("fs", "tp"),
        P("tp"),
        P("tp", "fs"),
        P(),
        P(),
    )
    out_specs = P(("grp", "fs"), None)
    sizes = tuple(mesh.shape[a] for a in ("grp", "fs", "tp"))
    chosen = quad_body if sizes == (2, 4, 4) else body
    return jax.shard_map(chosen, mesh=mesh, in_specs=in_specs, out_specs=out_specs, check_vma=False)
```
